32 devices in a mesh: sp: 4 (over z), fs: 4 (over y, x), tp: 2 (over core).
Axes of the slice: x: 2, y: 2, z: 4, core: 2. Of those that a mesh axis runs over, the one named last changes fastest.
Arguments:
- tokens: bfloat16 [4, 1024, 2048], P('fs', ('sp', 'tp')), may hold values from -6 to 6
- norm_gain: float32 [2048], replicated, may hold values from 0.1 to 1.9
- w_conv_gate: bfloat16 [2048, 1024], P('sp', 'tp'), may hold values from -0.125 to 0.125
- w_conv_in: bfloat16 [2048, 1024], P('sp', 'tp'), may hold values from -0.125 to 0.125
- w_conv_value: bfloat16 [2048, 1024], P('sp', 'tp'), may hold values from -0.125 to 0.125
- conv_taps: float32 [3, 1024], P(None, 'tp'), may hold values from -3.5 to 3.5
- w_receptance: bfloat16 [2048, 1024], P('sp', 'tp'), may hold values from -0.125 to 0.125
- w_key: bfloat16 [2048, 1024], P('sp', 'tp'), may hold values from -0.125 to 0.125
- w_value: bfloat16 [2048, 1024], P('sp', 'tp'), may hold values from -0.125 to 0.125
- w_decay_down: bfloat16 [2048, 128], P('sp'), may hold values from -0.125 to 0.125
- w_decay_up: bfloat16 [128, 1024], P(None, 'tp'), may hold values from -0.75 to 0.75
- decay_base: float32 [1024], P('tp'), may hold values from -12.5 to -3
- decay_shift: float32 [4, 1024, 1024], P('fs', 'sp', 'tp'), may hold values from -2.1 to 0
- w_rate_down: bfloat16 [2048, 128], P('sp'), may hold values from -0.125 to 0.125
- w_rate_up: bfloat16 [128, 1024], P(None, 'tp'), may hold values from -0.5 to 0.5
- rate_base: float32 [1024], P('tp'), may hold values from -10 to 1
- key_scale: float32 [1024], P('tp'), may hold values from 0.25 to 2.5
- key_mix: float32 [1024], P('tp'), may hold values from 0.1 to 0.7
- group_gain: float32 [1024], P('tp'), may hold values from 0.1 to 1.9
- w_out_conv: bfloat16 [1024, 2048], P('tp', 'sp'), may hold values from -0.125 to 0.125
- w_out_state: bfloat16 [1024, 2048], P('tp', 'sp'), may hold values from -0.125 to 0.125
Outputs:
- mixed: bfloat16 [4, 1024, 2048], P('fs', ('sp', 'tp'))
The draws below stay inside these ranges and needn't reach their ends.
All inputs are finite; a program needn't handle non-finite values.
Results may differ from the reference program's by a relative error of at most 0.015.
Values may be sent and summed in bfloat16 or wider, within the bound.
A program may use at most 128 MiB of HBM per device.

```python
import math
import jax
import jax.numpy as jnp
from jax import lax

D = 2048
CONV_CH = 1024
HEADS = 16
HEAD = 64
DECAY_RANK = 128
RATE_RANK = 128
TOK_DEV = 256
STATE_CH = 1024
SERIES_STEPS = 1024
BATCH_SERIES = 4
N_TP = 2


def quick_head_count(key):
    head_count = STATE_CH // HEAD
    order = jax.random.permutation(jax.random.fold_in(key, 101), head_count)
    chosen = order < head_count // 2
    return jnp.repeat(chosen, HEAD)


def draw_decay_base(key, part):
    jitter = jax.random.uniform(jax.random.fold_in(key, 202), (STATE_CH,), jnp.float32, -0.5, 0.5)
    return jnp.where(quick_head_count(key), -3.5 + jitter, -12.0 + jitter)


def draw_rate_base(key, part):
    quick = jax.random.uniform(jax.random.fold_in(key, 303), (STATE_CH,), jnp.float32, -1.0, 1.0)
    slower = jax.random.uniform(jax.random.fold_in(key, 404), (STATE_CH,), jnp.float32, -10.0, -8.0)
    return jnp.where(quick_head_count(key), quick, slower)


def draw_decay_shift(key, part):
    block_count = SERIES_STEPS // TOK_DEV
    levels = jnp.exp(jax.random.uniform(jax.random.fold_in(key, 505), (BATCH_SERIES, block_count, 1, 1), jnp.float32, math.log(3e-06), math.log(6e-05)))
    rough = jnp.exp(jax.random.uniform(jax.random.fold_in(key, 606), (BATCH_SERIES, block_count, TOK_DEV, STATE_CH), jnp.float32, math.log(0.5), math.log(2.0)))
    drift = -(levels * rough).reshape(BATCH_SERIES, SERIES_STEPS, STATE_CH)
    spike_location = jax.random.randint(jax.random.fold_in(key, 707), (BATCH_SERIES, 3), 0, SERIES_STEPS)
    losses = jnp.log(jax.random.uniform(jax.random.fold_in(key, 808), (BATCH_SERIES, 3, STATE_CH), jnp.float32, 0.5, 0.8))
    slot_numbers = jnp.arange(SERIES_STEPS)
    spike_total = (slot_numbers[None, None, :] == spike_location[:, :, None]).astype(jnp.float32)
    return drift + jnp.einsum('sbl,sbc->slc', spike_total, losses)


def level_of(key, dims, split, low, high):
    loudness, own = 1.0, jax.random.fold_in(key, 6)
    for dim, blocks in split:
        heights = jnp.exp(jax.random.uniform(jax.random.fold_in(own, dim), (blocks,), jnp.float32, low / len(split), high / len(split)))
        loudness = loudness * jnp.repeat(heights, dims[dim] // blocks).reshape([-1 if axis == dim else 1 for axis in range(len(dims))])
    return loudness


def scatter_about(rng, extent, width, bound, cuts=(), kind=jnp.bfloat16):
    factor_of = level_of(rng, extent, cuts, -0.22, 0.18) if cuts else 1.0
    entries = jax.random.normal(rng, extent, jnp.float32) * width * factor_of
    return jnp.minimum(jnp.maximum(entries, -bound), bound).astype(kind)


def setup_inputs(seed: int = 0) -> dict:
    streams_of = jax.random.split(jax.random.key(seed), 22)
    return {
        "tokens": scatter_about(streams_of[0], (BATCH_SERIES, SERIES_STEPS, D), 1.0, 6.0, ((0, 4), (1, 8))),
        "norm_gain": jnp.clip(1.0 + 0.18 * jax.random.normal(streams_of[1], (D,), jnp.float32), 0.1, 1.9),
        "w_conv_gate": scatter_about(streams_of[2], (D, CONV_CH), D ** -0.5, 0.125, ((0, 4), (1, 2))),
        "w_conv_in": scatter_about(streams_of[3], (D, CONV_CH), D ** -0.5, 0.125, ((0, 4), (1, 2))),
        "w_conv_value": scatter_about(streams_of[4], (D, CONV_CH), D ** -0.5, 0.125, ((0, 4), (1, 2))),
        "conv_taps": scatter_about(streams_of[5], (3, CONV_CH), 3 ** -0.5, 3.5, ((1, 2),), jnp.float32),
        "w_receptance": scatter_about(streams_of[6], (D, STATE_CH), D ** -0.5, 0.125, ((0, 4), (1, 2))),
        "w_key": scatter_about(streams_of[7], (D, STATE_CH), D ** -0.5, 0.125, ((0, 4), (1, 2))),
        "w_value": scatter_about(streams_of[8], (D, STATE_CH), D ** -0.5, 0.125, ((0, 4), (1, 2))),
        "w_decay_down": scatter_about(streams_of[9], (D, DECAY_RANK), D ** -0.5, 0.125, ((0, 4),)),
        "w_decay_up": scatter_about(streams_of[10], (DECAY_RANK, STATE_CH), (DECAY_RANK // 2) ** -0.5, 0.75, ((1, 2),)),
        "decay_base": draw_decay_base(jax.random.fold_in(streams_of[21], 71), 0),
        "decay_shift": draw_decay_shift(jax.random.fold_in(streams_of[21], 71), 0),
        "w_rate_down": scatter_about(streams_of[13], (D, RATE_RANK), D ** -0.5, 0.125, ((0, 4),)),
        "w_rate_up": scatter_about(streams_of[14], (RATE_RANK, STATE_CH), RATE_RANK ** -0.5, 0.5, ((1, 2),)),
        "rate_base": draw_rate_base(jax.random.fold_in(streams_of[21], 71), 0),
        "key_scale": jnp.clip(jnp.exp(math.log(2.5) - 2.3025851 * jax.random.uniform(streams_of[16], (STATE_CH,), jnp.float32) ** level_of(streams_of[16], (STATE_CH,), ((0, 2),), -0.2, 0.2)), 0.25, 2.5),
        "key_mix": jnp.clip(0.1 + 0.59999999 * jax.random.uniform(streams_of[17], (STATE_CH,), jnp.float32) ** level_of(streams_of[17], (STATE_CH,), ((0, 2),), -0.2, 0.2), 0.1, 0.7),
        "group_gain": jnp.clip(1.0 + 0.18 * jax.random.normal(streams_of[18], (STATE_CH,), jnp.float32), 0.1, 1.9),
        "w_out_conv": scatter_about(streams_of[19], (CONV_CH, D), (CONV_CH + STATE_CH) ** -0.5, 0.125, ((0, 2), (1, 4))),
        "w_out_state": scatter_about(streams_of[20], (STATE_CH, D), (CONV_CH + STATE_CH) ** -0.5, 0.125, ((0, 2), (1, 4))),
    }


highest = lax.Precision.HIGHEST

def normalize_rows(rows_in, norm_gain):
    values = rows_in.astype(jnp.float32)
    scaled = values * lax.rsqrt(lax.optimization_barrier(jnp.mean(values * values, axis=-1, keepdims=True)) + 1e-06)
    return (scaled * norm_gain).astype(jnp.bfloat16)

def project(normed, weight):
    return jnp.dot(normed, weight, preferred_element_type=jnp.float32).astype(jnp.bfloat16)

def recurrence(receptance, decay_mul, key_write, value_vec, erase_vec, replace_vec):

    def advance(memory, inputs_now):
        recv_now, decay_now, key_now, value_now, erase_now, replace_now = inputs_now
        erased = jnp.einsum('hvk,hk->hv', memory, erase_now, precision=highest)
        memory = memory * decay_now[:, None, :] + erased[:, :, None] * replace_now[:, None, :] + value_now[:, :, None] * key_now[:, None, :]
        return (memory, jnp.einsum('hvk,hk->hv', memory, recv_now, precision=highest))
    initial = jnp.zeros((HEADS, HEAD, HEAD), jnp.float32)
    return lax.scan(advance, initial, (receptance, decay_mul, key_write, value_vec, erase_vec, replace_vec))[1]

def merge_outputs(conv_out, state_out, w_out_conv, w_out_state):
    filter_branch_output = CONV_CH // N_TP
    state_part = STATE_CH // N_TP
    combined = jnp.zeros((conv_out.shape[0], w_out_conv.shape[1]), jnp.float32)
    for member in range(N_TP):
        conv_lo = member * filter_branch_output
        state_lo = member * state_part
        partial_sum = jnp.dot(conv_out[:, conv_lo:conv_lo + filter_branch_output], w_out_conv[conv_lo:conv_lo + filter_branch_output], preferred_element_type=jnp.float32) + jnp.dot(state_out[:, state_lo:state_lo + state_part], w_out_state[state_lo:state_lo + state_part], preferred_element_type=jnp.float32)
        rounded = lax.optimization_barrier(partial_sum.astype(jnp.bfloat16))
        combined = combined + rounded.astype(jnp.float32)
    return combined.astype(jnp.bfloat16)

def split_heads(values):
    return values.reshape(values.shape[0], HEADS, HEAD)

def reference(tokens, norm_gain, w_conv_gate, w_conv_in, w_conv_value, conv_taps, w_receptance, w_key, w_value, w_decay_down, w_decay_up, decay_base, decay_shift, w_rate_down, w_rate_up, rate_base, key_scale, key_mix, group_gain, w_out_conv, w_out_state):
    results = []
    for sequence in range(BATCH_SERIES):
        normed = normalize_rows(tokens[sequence], norm_gain)
        conv_gate = project(normed, w_conv_gate)
        filter_source = project(normed, w_conv_in)
        conv_value = project(normed, w_conv_value)
        product_value = filter_source.astype(jnp.float32) * conv_value.astype(jnp.float32)
        padded = jnp.concatenate([jnp.zeros((2, CONV_CH), jnp.float32), product_value], axis=0)
        filtered = conv_taps[0] * padded[:-2] + conv_taps[1] * padded[1:-1] + conv_taps[2] * padded[2:]
        conv_out = (conv_gate.astype(jnp.float32) * filtered).astype(jnp.bfloat16)
        receptance = project(normed, w_receptance)
        key_raw = project(normed, w_key)
        value_raw = project(normed, w_value)
        decay_low = project(normed, w_decay_down)
        rate_low = project(normed, w_rate_down)
        decay_act = jnp.tanh(decay_low.astype(jnp.float32)).astype(jnp.bfloat16)
        decay_pre = decay_base + jnp.dot(decay_act, w_decay_up, preferred_element_type=jnp.float32)
        log_decay = decay_shift[sequence] - jnp.exp(-jax.nn.softplus(-decay_pre) - 0.5)
        learn_rate = jax.nn.sigmoid(rate_base + jnp.dot(rate_low, w_rate_up, preferred_element_type=jnp.float32))
        scaled_key = split_heads(key_raw.astype(jnp.float32) * key_scale)
        erase_dir = scaled_key * lax.rsqrt(lax.optimization_barrier(jnp.sum(scaled_key * scaled_key, axis=-1, keepdims=True)) + 1e-06)
        key_write = key_raw.astype(jnp.float32) * (1.0 + (learn_rate - 1.0) * key_mix)
        readouts = recurrence(split_heads(receptance.astype(jnp.float32)), split_heads(jnp.exp(log_decay)), split_heads(key_write), split_heads(value_raw.astype(jnp.float32)), -erase_dir, erase_dir * split_heads(learn_rate))
        centered = readouts - lax.optimization_barrier(jnp.mean(readouts, axis=-1, keepdims=True))
        variance = lax.optimization_barrier(jnp.mean(centered * centered, axis=-1, keepdims=True))
        normal_heads = (centered * lax.rsqrt(variance + 0.00064)).reshape(SERIES_STEPS, STATE_CH)
        state_out = (normal_heads * group_gain).astype(jnp.bfloat16)
        results.append(merge_outputs(conv_out, state_out, w_out_conv, w_out_state))
    return jnp.stack(results)
```

```python
import functools

import jax
import jax.numpy as jnp
from jax import lax
from jax.experimental import pallas as pl
from jax.experimental.pallas import tpu as pltpu
from jax.sharding import PartitionSpec as P

HEAD = 64
CHUNK = 64
norm_eps = 1e-06
group_eps = 0.00064
f32, bf16 = jnp.float32, jnp.bfloat16

NN = (((1,), (0,)), ((), ()))
NT = (((1,), (1,)), ((), ()))
TN = (((0,), (0,)), ((), ()))


def dot1(a, b, dims):
    return lax.dot_general(a.astype(bf16), b.astype(bf16), dims, preferred_element_type=f32)


def dot3(a, b, dims):
    ah, bh = a.astype(bf16), b.astype(bf16)
    al, bl = (a - ah.astype(f32)).astype(bf16), (b - bh.astype(f32)).astype(bf16)
    d = functools.partial(lax.dot_general, dimension_numbers=dims, preferred_element_type=f32)
    return d(ah, bh) + (d(ah, bl) + d(al, bh))


def stack_heads(x, lanes_low):
    return jnp.concatenate([jnp.where(lanes_low, x, 0.0), jnp.where(lanes_low, 0.0, x)], axis=0)


def fold(x):
    half = x.shape[0] // 2
    return x[:half] + x[half:]


def state_kernel(
    recv_ref, key_ref, val_ref, dlow_ref, rlow_ref, wdu_ref, wru_ref, shift_ref, par_ref,
    q_ref, l_ref, ma_ref,
):
    tokens, width = recv_ref.shape
    par = par_ref[...]
    decay_base, rate_base, key_scale, key_mix = (par[i : i + 1] for i in range(4))
    act = jnp.tanh(dlow_ref[...].astype(f32)).astype(bf16)
    pre = decay_base + lax.dot_general(act, wdu_ref[...], NN, preferred_element_type=f32)
    log_decay = shift_ref[0] - jnp.exp(-0.5) * jax.nn.sigmoid(pre)
    rate = jax.nn.sigmoid(
        rate_base + lax.dot_general(rlow_ref[...], wru_ref[...], NN, preferred_element_type=f32)
    )
    key = key_ref[...].astype(f32)
    scaled = key * key_scale
    lane_low = lax.broadcasted_iota(jnp.int32, (1, width), 1) < HEAD
    sq = scaled * scaled
    low_sum = jnp.sum(jnp.where(lane_low, sq, 0.0), axis=-1, keepdims=True)
    high_sum = jnp.sum(jnp.where(lane_low, 0.0, sq), axis=-1, keepdims=True)
    erase = scaled * lax.rsqrt(jnp.where(lane_low, low_sum, high_sum) + norm_eps)
    write = key * (1.0 + (rate - 1.0) * key_mix)
    replace = erase * rate
    recv = recv_ref[...].astype(f32)
    val = val_ref[...].astype(f32)

    rows = 2 * CHUNK
    ri = lax.broadcasted_iota(jnp.int32, (rows, rows), 0)
    ci = lax.broadcasted_iota(jnp.int32, (rows, rows), 1)
    same = (ri < CHUNK) == (ci < CHUNK)
    strict = jnp.logical_and(same, ri > ci)
    causal = jnp.logical_and(same, ri >= ci)
    eye = (ri == ci).astype(f32)
    tri = jnp.where(
        lax.broadcasted_iota(jnp.int32, (CHUNK, CHUNK), 0)
        >= lax.broadcasted_iota(jnp.int32, (CHUNK, CHUNK), 1),
        1.0,
        0.0,
    ).astype(f32)
    wi = lax.broadcasted_iota(jnp.int32, (width, width), 0)
    wj = lax.broadcasted_iota(jnp.int32, (width, width), 1)
    weye = wi == wj

    parts = []
    for c in range(tokens // CHUNK):
        sl = slice(c * CHUNK, (c + 1) * CHUNK)
        ld = log_decay[sl]
        incl = lax.dot_general(tri, ld, NN, precision=lax.Precision.HIGHEST, preferred_element_type=f32)
        final = incl[CHUNK - 1 : CHUNK]
        mid = incl[CHUNK // 2 - 1 : CHUNK // 2]
        excl = incl - ld
        up, back = jnp.exp(incl - mid), jnp.exp(mid - incl)
        st = lambda x: stack_heads(x, lane_low)
        e_mid = st(-erase[sl] * jnp.exp(excl - mid))
        q_mid = st(recv[sl] * up)
        r_back = st(replace[sl] * back)
        k_back = st(write[sl] * back)
        v = st(val[sl])
        e_now = st(-erase[sl] * jnp.exp(excl))
        q_now = st(recv[sl] * jnp.exp(incl))
        tail = jnp.exp(final - incl)
        r_end = st(replace[sl] * tail)
        k_end = st(write[sl] * tail)
        x = jnp.where(strict, dot3(e_mid, r_back, NT), 0.0)
        ek = jnp.where(strict, dot1(e_mid, k_back, NT), 0.0)
        qr = jnp.where(causal, dot1(q_mid, r_back, NT), 0.0)
        qk = jnp.where(causal, dot1(q_mid, k_back, NT), 0.0)
        inv = eye + x
        power = x
        reached = 2
        while reached < CHUNK:
            power = dot3(power, power, NN)
            inv = inv + dot3(inv, power, NN)
            reached *= 2
        start_map = dot3(inv, e_now, NN)
        local_erase = dot1(inv, dot1(ek, v, NN), NN)
        query_map = fold(q_now + dot1(qr, start_map, NN))
        local_out = fold(dot1(qr, local_erase, NN) + dot1(qk, v, NN))
        decay_diag = jnp.where(weye, jnp.exp(final), 0.0)
        step_map = decay_diag + dot3(start_map, r_end, TN)
        carried = dot1(local_erase, r_end, TN) + dot1(v, k_end, TN)
        parts.append((query_map, local_out, step_map, carried))

    total_map = total_add = None
    for c, (query_map, local_out, step_map, carried) in enumerate(parts):
        sl = slice(c * CHUNK, (c + 1) * CHUNK)
        if c == 0:
            q_ref[sl] = query_map.astype(bf16)
            l_ref[sl] = local_out
            total_map, total_add = step_map, carried
        else:
            q_ref[sl] = dot1(query_map, total_map, NT).astype(bf16)
            l_ref[sl] = local_out + dot1(query_map, total_add, NT)
            total_map, total_add = (
                dot3(total_map, step_map, NN),
                dot3(total_add, step_map, NN) + carried,
            )
    ma_ref[0, 0] = fold(total_map).astype(bf16)
    ma_ref[0, 1] = fold(total_add).astype(bf16)


def finish_kernel(n_sp, place_ref, q_ref, l_ref, ma_ref, gain_ref, out_ref):
    width = q_ref.shape[1]
    place = place_ref[0]
    wi = lax.broadcasted_iota(jnp.int32, (width, width), 0)
    wj = lax.broadcasted_iota(jnp.int32, (width, width), 1)
    same = (wi < HEAD) == (wj < HEAD)
    widen = lambda x: jnp.where(same, jnp.concatenate([x, x], axis=0), 0.0)
    state = jnp.zeros((width, width), f32)
    for hop in range(n_sp - 1):
        new = dot3(state, widen(ma_ref[hop, 0, 0].astype(f32)), NN) + widen(
            ma_ref[hop, 0, 1].astype(f32)
        )
        state = jnp.where(hop < place, new, state)
    out = l_ref[...] + dot1(q_ref[...], state, NT)
    low = lax.broadcasted_iota(jnp.int32, (1, width), 1) < HEAD

    def head_mean(x):
        a = jnp.sum(jnp.where(low, x, 0.0), axis=-1, keepdims=True)
        b = jnp.sum(jnp.where(low, 0.0, x), axis=-1, keepdims=True)
        return jnp.where(low, a, b) * (1.0 / HEAD)

    centered = out - head_mean(out)
    var = head_mean(centered * centered)
    out_ref[...] = (centered * lax.rsqrt(var + group_eps) * gain_ref[...]).astype(bf16)


def normalize_rows(norm_gain, row_piece):
    values = row_piece.astype(f32)
    scaled = values * lax.rsqrt(jnp.mean(values * values, axis=-1, keepdims=True) + norm_eps)
    return (scaled * norm_gain).astype(bf16)


def body(
    tokens, norm_gain, w_conv_gate, w_conv_in, w_conv_value, conv_taps, w_receptance, w_key,
    w_value, w_decay_down, w_decay_up, decay_base, decay_shift, w_rate_down, w_rate_up,
    rate_base, key_scale, key_mix, group_gain, w_out_conv, w_out_state,
):
    n_fs, n_sp = lax.axis_size("fs"), lax.axis_size("sp")
    fs = lax.axis_index("fs")
    width = w_key.shape[1] // n_fs

    def mine(a, axis):
        return lax.dynamic_slice_in_dim(a, fs * width, width, axis)

    normed = lax.all_gather(normalize_rows(norm_gain, tokens[0]), ("fs", "tp"), axis=0, tiled=True)
    steps = normed.shape[0] // n_fs
    w_state = jnp.concatenate(
        [mine(w_receptance, 1), mine(w_key, 1), mine(w_value, 1), w_decay_down, w_rate_down], axis=1
    )
    w_conv = jnp.concatenate([mine(w_conv_gate, 1), mine(w_conv_in, 1), mine(w_conv_value, 1)], axis=1)
    w_out = jnp.concatenate([mine(w_out_conv, 0), mine(w_out_state, 0)], axis=0)
    w_state = lax.all_gather(w_state, "sp", axis=0, tiled=True)
    w_conv = lax.all_gather(w_conv, "sp", axis=0, tiled=True)
    w_out = lax.all_gather(w_out, "sp", axis=0)
    shift = lax.all_to_all(
        decay_shift[0].reshape(steps, n_fs, width), "fs", split_axis=1, concat_axis=0
    ).reshape(n_fs, steps, width)

    state_in = jnp.dot(normed, w_state, preferred_element_type=f32).astype(bf16)
    params = jnp.stack([mine(p, 0) for p in (decay_base, rate_base, key_scale, key_mix)])
    rank = w_decay_down.shape[1]
    col = lambda k: pl.BlockSpec((steps, width), lambda i, k=k: (i, k))
    low = lambda k: pl.BlockSpec((steps, rank), lambda i, k=k: (i, 3 * width // rank + k))
    full = lambda s: pl.BlockSpec(s, lambda i: (0,) * len(s))
    query, local, ma = pl.pallas_call(
        state_kernel,
        grid=(n_fs,),
        in_specs=[
            col(0), col(1), col(2), low(0), low(1), full((rank, width)), full((rank, width)),
            pl.BlockSpec((1, steps, width), lambda i: (i, 0, 0)), full((4, width)),
        ],
        out_specs=[
            col(0), col(0), pl.BlockSpec((1, 2, HEAD, width), lambda i: (i, 0, 0, 0)),
        ],
        out_shape=[
            jax.ShapeDtypeStruct((n_fs * steps, width), bf16),
            jax.ShapeDtypeStruct((n_fs * steps, width), f32),
            jax.ShapeDtypeStruct((n_fs, 2, HEAD, width), bf16),
        ],
        cost_estimate=pl.CostEstimate(flops=40_000_000_000, bytes_accessed=4_000_000, transcendentals=0),
    )(
        state_in, state_in, state_in, state_in, state_in, mine(w_decay_up, 1), mine(w_rate_up, 1),
        shift, params,
    )
    ma_all = lax.all_gather(ma, "sp", axis=0)

    conv = jnp.dot(normed, w_conv, preferred_element_type=f32).astype(bf16)
    gate, source, value = (
        conv[:, i * width : (i + 1) * width].reshape(n_fs, steps, width) for i in range(3)
    )
    route = [(i, i + 1) for i in range(n_sp - 1)]
    previous = lax.ppermute(jnp.stack([source[:, -2:], value[:, -2:]]), "sp", route)
    product = jnp.concatenate([previous[0], source], axis=1).astype(f32) * jnp.concatenate(
        [previous[1], value], axis=1
    ).astype(f32)
    taps = mine(conv_taps, 1)
    filtered = taps[0] * product[:, :-2] + taps[1] * product[:, 1:-1] + taps[2] * product[:, 2:]
    conv_out = (gate.astype(f32) * filtered).astype(bf16).reshape(n_fs * steps, width)

    state_out = pl.pallas_call(
        functools.partial(finish_kernel, n_sp),
        grid=(n_fs,),
        in_specs=[
            pl.BlockSpec(memory_space=pltpu.SMEM), col(0), col(0),
            pl.BlockSpec((n_sp, 1, 2, HEAD, width), lambda i: (0, i, 0, 0, 0)), full((1, width)),
        ],
        out_specs=col(0),
        out_shape=jax.ShapeDtypeStruct((n_fs * steps, width), bf16),
    )(lax.axis_index("sp").reshape(1), query, local, ma_all, mine(group_gain, 0)[None])

    both = jnp.concatenate([conv_out, state_out], axis=1)
    partial = jnp.concatenate(
        [jnp.dot(both, w_out[j], preferred_element_type=f32).astype(bf16) for j in range(n_sp)], axis=1
    )
    mixed = lax.psum_scatter(partial, ("fs", "tp"), scatter_dimension=0, tiled=True)
    return mixed[None]


def solution(mesh):
    in_specs = (
        P("fs", ("sp", "tp"), None), P(), P("sp", "tp"), P("sp", "tp"), P("sp", "tp"),
        P(None, "tp"), P("sp", "tp"), P("sp", "tp"), P("sp", "tp"), P("sp", None), P(None, "tp"),
        P("tp"), P("fs", "sp", "tp"), P("sp", None), P(None, "tp"), P("tp"), P("tp"), P("tp"),
        P("tp"), P("tp", "sp"), P("tp", "sp"),
    )
    out_specs = P("fs", ("sp", "tp"), None)
    return jax.shard_map(body, mesh=mesh, in_specs=in_specs, out_specs=out_specs, check_vma=False)
```

```python
import functools

import jax
import jax.numpy as jnp
from jax import lax
from jax.experimental import pallas as pl
from jax.experimental.pallas import tpu as pltpu
from jax.sharding import PartitionSpec as P

HEAD = 64
CHUNK = 64
norm_eps = 1e-06
group_eps = 0.00064
f32, bf16 = jnp.float32, jnp.bfloat16

NN = (((1,), (0,)), ((), ()))
NT = (((1,), (1,)), ((), ()))
TN = (((0,), (0,)), ((), ()))


def dot1(a, b, dims):
    return lax.dot_general(a.astype(bf16), b.astype(bf16), dims, preferred_element_type=f32)


def dot3(a, b, dims):
    ah, bh = a.astype(bf16), b.astype(bf16)
    al, bl = (a - ah.astype(f32)).astype(bf16), (b - bh.astype(f32)).astype(bf16)
    d = functools.partial(lax.dot_general, dimension_numbers=dims, preferred_element_type=f32)
    return d(ah, bh) + (d(ah, bl) + d(al, bh))


def stack_heads(x, lanes_low):
    return jnp.concatenate([jnp.where(lanes_low, x, 0.0), jnp.where(lanes_low, 0.0, x)], axis=0)


def fold(x):
    half = x.shape[0] // 2
    return x[:half] + x[half:]


def state_kernel(
    recv_ref, key_ref, val_ref, dlow_ref, rlow_ref, wdu_ref, wru_ref, shift_ref, par_ref,
    q_ref, l_ref, ma_ref,
):
    tokens, width = recv_ref.shape
    par = par_ref[...]
    decay_base, rate_base, key_scale, key_mix = (par[i : i + 1] for i in range(4))
    act = jnp.tanh(dlow_ref[...].astype(f32)).astype(bf16)
    pre = decay_base + lax.dot_general(act, wdu_ref[...], NN, preferred_element_type=f32)
    log_decay = shift_ref[0] - jnp.exp(-0.5) * jax.nn.sigmoid(pre)
    rate = jax.nn.sigmoid(
        rate_base + lax.dot_general(rlow_ref[...], wru_ref[...], NN, preferred_element_type=f32)
    )
    key = key_ref[...].astype(f32)
    scaled = key * key_scale
    lane_low = lax.broadcasted_iota(jnp.int32, (1, width), 1) < HEAD
    sq = scaled * scaled
    low_sum = jnp.sum(jnp.where(lane_low, sq, 0.0), axis=-1, keepdims=True)
    high_sum = jnp.sum(jnp.where(lane_low, 0.0, sq), axis=-1, keepdims=True)
    erase = scaled * lax.rsqrt(jnp.where(lane_low, low_sum, high_sum) + norm_eps)
    write = key * (1.0 + (rate - 1.0) * key_mix)
    replace = erase * rate
    recv = recv_ref[...].astype(f32)
    val = val_ref[...].astype(f32)

    rows = 2 * CHUNK
    ri = lax.broadcasted_iota(jnp.int32, (rows, rows), 0)
    ci = lax.broadcasted_iota(jnp.int32, (rows, rows), 1)
    same = (ri < CHUNK) == (ci < CHUNK)
    strict = jnp.logical_and(same, ri > ci)
    causal = jnp.logical_and(same, ri >= ci)
    eye = (ri == ci).astype(f32)
    tri = jnp.where(
        lax.broadcasted_iota(jnp.int32, (CHUNK, CHUNK), 0)
        >= lax.broadcasted_iota(jnp.int32, (CHUNK, CHUNK), 1),
        1.0,
        0.0,
    ).astype(f32)
    wi = lax.broadcasted_iota(jnp.int32, (width, width), 0)
    wj = lax.broadcasted_iota(jnp.int32, (width, width), 1)
    weye = wi == wj

    parts = []
    for c in range(tokens // CHUNK):
        sl = slice(c * CHUNK, (c + 1) * CHUNK)
        ld = log_decay[sl]
        incl = lax.dot_general(tri, ld, NN, precision=lax.Precision.HIGHEST, preferred_element_type=f32)
        final = incl[CHUNK - 1 : CHUNK]
        mid = incl[CHUNK // 2 - 1 : CHUNK // 2]
        excl = incl - ld
        up, back = jnp.exp(incl - mid), jnp.exp(mid - incl)
        st = lambda x: stack_heads(x, lane_low)
        e_mid = st(-erase[sl] * jnp.exp(excl - mid))
        q_mid = st(recv[sl] * up)
        r_back = st(replace[sl] * back)
        k_back = st(write[sl] * back)
        v = st(val[sl])
        e_now = st(-erase[sl] * jnp.exp(excl))
        q_now = st(recv[sl] * jnp.exp(incl))
        tail = jnp.exp(final - incl)
        r_end = st(replace[sl] * tail)
        k_end = st(write[sl] * tail)
        x = jnp.where(strict, dot3(e_mid, r_back, NT), 0.0)
        ek = jnp.where(strict, dot1(e_mid, k_back, NT), 0.0)
        qr = jnp.where(causal, dot1(q_mid, r_back, NT), 0.0)
        qk = jnp.where(causal, dot1(q_mid, k_back, NT), 0.0)
        inv = eye + x
        power = x
        reached = 2
        while reached < CHUNK:
            power = dot3(power, power, NN)
            inv = inv + dot3(inv, power, NN)
            reached *= 2
        start_map = dot3(inv, e_now, NN)
        local_erase = dot1(inv, dot1(ek, v, NN), NN)
        query_map = fold(q_now + dot1(qr, start_map, NN))
        local_out = fold(dot1(qr, local_erase, NN) + dot1(qk, v, NN))
        decay_diag = jnp.where(weye, jnp.exp(final), 0.0)
        step_map = decay_diag + dot3(start_map, r_end, TN)
        carried = dot1(local_erase, r_end, TN) + dot1(v, k_end, TN)
        parts.append((query_map, local_out, step_map, carried))

    total_map = total_add = None
    for c, (query_map, local_out, step_map, carried) in enumerate(parts):
        sl = slice(c * CHUNK, (c + 1) * CHUNK)
        if c == 0:
            q_ref[sl] = query_map.astype(bf16)
            l_ref[sl] = local_out
            total_map, total_add = step_map, carried
        else:
            q_ref[sl] = dot1(query_map, total_map, NT).astype(bf16)
            l_ref[sl] = local_out + dot1(query_map, total_add, NT)
            total_map, total_add = (
                dot3(total_map, step_map, NN),
                dot3(total_add, step_map, NN) + carried,
            )
    ma_ref[0, 0] = fold(total_map).astype(bf16)
    ma_ref[0, 1] = fold(total_add).astype(bf16)


def finish_kernel(n_sp, place_ref, q_ref, l_ref, ma_ref, gain_ref, out_ref):
    width = q_ref.shape[1]
    place = place_ref[0]
    wi = lax.broadcasted_iota(jnp.int32, (width, width), 0)
    wj = lax.broadcasted_iota(jnp.int32, (width, width), 1)
    same = (wi < HEAD) == (wj < HEAD)
    widen = lambda x: jnp.where(same, jnp.concatenate([x, x], axis=0), 0.0)
    state = jnp.zeros((width, width), f32)
    for hop in range(n_sp - 1):
        new = dot3(state, widen(ma_ref[hop, 0, 0].astype(f32)), NN) + widen(
            ma_ref[hop, 0, 1].astype(f32)
        )
        state = jnp.where(hop < place, new, state)
    out = l_ref[...] + dot1(q_ref[...], state, NT)
    low = lax.broadcasted_iota(jnp.int32, (1, width), 1) < HEAD

    def head_mean(x):
        a = jnp.sum(jnp.where(low, x, 0.0), axis=-1, keepdims=True)
        b = jnp.sum(jnp.where(low, 0.0, x), axis=-1, keepdims=True)
        return jnp.where(low, a, b) * (1.0 / HEAD)

    centered = out - head_mean(out)
    var = head_mean(centered * centered)
    out_ref[...] = (centered * lax.rsqrt(var + group_eps) * gain_ref[...]).astype(bf16)


MESH = pl.DeviceIdType.MESH


def greet(peers):
    barrier = pltpu.get_barrier_semaphore()
    for peer in peers:
        pl.semaphore_signal(barrier, inc=1, device_id=peer, device_id_type=MESH)
    return barrier


def send(src, dst, send_sem, recv_sem, peer):
    return pltpu.make_async_remote_copy(
        src_ref=src, dst_ref=dst, send_sem=send_sem, recv_sem=recv_sem,
        device_id=peer, device_id_type=MESH,
    )


def gather_kernel(
    n_sp, n_fs, tok_ref, w_ref, toks, weights, local_sem, tok_send, tok_recv, pair_send, pair_recv,
    right_send, left_send, w_recv,
):
    sp, fs, tp = lax.axis_index("sp"), lax.axis_index("fs"), lax.axis_index("tp")
    partner = {"tp": 1 - tp}
    others = [lax.rem(fs + d, n_fs) for d in range(1, n_fs)]
    barrier = greet([partner] + [{"fs": f} for f in others])
    has_left, has_right = sp > 0, sp < n_sp - 1

    @pl.when(has_left)
    def _():
        pl.semaphore_signal(barrier, inc=1, device_id={"sp": sp - 1}, device_id_type=MESH)

    @pl.when(has_right)
    def _():
        pl.semaphore_signal(barrier, inc=1, device_id={"sp": sp + 1}, device_id_type=MESH)

    pl.semaphore_wait(barrier, n_fs + has_left.astype(jnp.int32) + has_right.astype(jnp.int32))

    def rightward(j):
        src = weights.at[j]
        return send(src, weights.at[j], right_send.at[j], w_recv.at[j], {"sp": sp + 1})

    def leftward(j):
        src = weights.at[j]
        return send(src, weights.at[j], left_send.at[j], w_recv.at[j], {"sp": sp - 1})

    own_right = send(w_ref, weights.at[sp], right_send.at[sp], w_recv.at[sp], {"sp": sp + 1})
    own_left = send(w_ref, weights.at[sp], left_send.at[sp], w_recv.at[sp], {"sp": sp - 1})

    @pl.when(has_right)
    def _():
        own_right.start()

    @pl.when(has_left)
    def _():
        own_left.start()

    own_w = pltpu.make_async_copy(w_ref, weights.at[sp], local_sem.at[0])
    own_t = pltpu.make_async_copy(tok_ref, toks.at[fs, tp], local_sem.at[1])
    own_w.start()
    own_t.start()
    token_sends = [
        send(tok_ref, toks.at[fs, tp], tok_send.at[f], tok_recv.at[fs], {"fs": f}) for f in others
    ]
    for copy in token_sends:
        copy.start()
    pair_own = send(tok_ref, toks.at[fs, tp], pair_send.at[fs], pair_recv.at[fs], partner)
    pair_own.start()

    def from_peer(f):
        return send(toks.at[f, tp], toks.at[f, tp], tok_send.at[f], tok_recv.at[f], {"fs": f})

    def to_partner(f):
        return send(toks.at[f, tp], toks.at[f, tp], pair_send.at[f], pair_recv.at[f], partner)

    def from_partner(f):
        there = toks.at[f, 1 - tp]
        return send(there, there, pair_send.at[f], pair_recv.at[f], partner)

    for k in range(1, n_sp):

        @pl.when(sp >= k)
        def _():
            rightward(sp - k).wait_recv()

            @pl.when(has_right)
            def _():
                rightward(sp - k).start()

        @pl.when(sp + k < n_sp)
        def _():
            leftward(sp + k).wait_recv()

            @pl.when(has_left)
            def _():
                leftward(sp + k).start()

        if k == 1:
            for f in reversed(others):
                from_peer(f).wait_recv()
                to_partner(f).start()

    own_w.wait()
    own_t.wait()
    for copy in token_sends:
        copy.wait_send()
    pair_own.wait_send()
    for f in others:
        to_partner(f).wait_send()
    for f in [fs] + others:
        from_partner(f).wait_recv()

    @pl.when(has_right)
    def _():
        own_right.wait_send()

    @pl.when(has_left)
    def _():
        own_left.wait_send()

    for k in range(1, n_sp):

        @pl.when(jnp.logical_and(sp >= k, has_right))
        def _():
            rightward(sp - k).wait_send()

        @pl.when(jnp.logical_and(sp + k < n_sp, has_left))
        def _():
            leftward(sp + k).wait_send()


def reduce_kernel(
    n_fs, part_ref, out_ref, from_pair, sums, from_fs, pair_send, pair_recv, fs_send, fs_recv
):
    fs, tp = lax.axis_index("fs"), lax.axis_index("tp")
    partner = {"tp": 1 - tp}
    order = [lax.rem(fs + d, n_fs) for d in range(1, n_fs)] + [fs]
    barrier = greet([partner] + [{"fs": f} for f in order[:-1]])
    pl.semaphore_wait(barrier, n_fs)
    swaps = [
        send(part_ref.at[f, 1 - tp], from_pair.at[d], pair_send.at[d], pair_recv.at[d], partner)
        for d, f in enumerate(order)
    ]
    for copy in swaps:
        copy.start()
    sends = []
    for d, f in enumerate(order):
        swaps[d].wait_recv()
        total = part_ref[f, tp].astype(f32) + from_pair[d].astype(f32)
        sums[d] = total.astype(bf16)
        if d < n_fs - 1:
            copy = send(sums.at[d], from_fs.at[d], fs_send.at[d], fs_recv.at[d], {"fs": f})
            copy.start()
            sends.append(copy)
    for copy in sends:
        copy.wait_recv()
    result = sums[n_fs - 1].astype(f32)
    for d in range(n_fs - 1):
        result = result + from_fs[d].astype(f32)
    out_ref[...] = result.astype(bf16)
    for copy in sends:
        copy.wait_send()
    for copy in swaps:
        copy.wait_send()


def gather_inputs(n_sp, n_fs, n_tp, tok, w):
    dma = lambda n: pltpu.SemaphoreType.DMA((n,))
    return pl.pallas_call(
        functools.partial(gather_kernel, n_sp, n_fs),
        in_specs=[pl.BlockSpec(memory_space=pltpu.VMEM)] * 2,
        out_specs=[pl.BlockSpec(memory_space=pltpu.VMEM)] * 2,
        out_shape=[
            jax.ShapeDtypeStruct((n_fs, n_tp) + tok.shape, bf16),
            jax.ShapeDtypeStruct((n_sp,) + w.shape, bf16),
        ],
        scratch_shapes=[dma(2), dma(n_fs), dma(n_fs), dma(n_fs), dma(n_fs), dma(n_sp), dma(n_sp), dma(n_sp)],
        compiler_params=pltpu.CompilerParams(collective_id=0, has_side_effects=True),
    )(tok, w)


def reduce_partials(n_fs, part):
    dma = pltpu.SemaphoreType.DMA((n_fs,))
    block = pltpu.VMEM((n_fs,) + part.shape[2:], bf16)
    return pl.pallas_call(
        functools.partial(reduce_kernel, n_fs),
        in_specs=[pl.BlockSpec(memory_space=pltpu.VMEM)],
        out_specs=pl.BlockSpec(memory_space=pltpu.VMEM),
        out_shape=jax.ShapeDtypeStruct(part.shape[2:], bf16),
        scratch_shapes=[block, block, block, dma, dma, dma, dma],
        compiler_params=pltpu.CompilerParams(collective_id=1, has_side_effects=True),
    )(part)


def normalize_rows(norm_gain, row_piece):
    values = row_piece.astype(f32)
    scaled = values * lax.rsqrt(jnp.mean(values * values, axis=-1, keepdims=True) + norm_eps)
    return (scaled * norm_gain).astype(bf16)


def body(
    tokens, norm_gain, w_conv_gate, w_conv_in, w_conv_value, conv_taps, w_receptance, w_key,
    w_value, w_decay_down, w_decay_up, decay_base, decay_shift, w_rate_down, w_rate_up,
    rate_base, key_scale, key_mix, group_gain, w_out_conv, w_out_state,
):
    n_fs, n_sp = lax.axis_size("fs"), lax.axis_size("sp")
    fs = lax.axis_index("fs")
    width = w_key.shape[1] // n_fs

    def mine(a, axis):
        return lax.dynamic_slice_in_dim(a, fs * width, width, axis)

    n_tp = lax.axis_size("tp")
    steps = decay_shift.shape[1]
    w_state = jnp.concatenate(
        [mine(w_receptance, 1), mine(w_key, 1), mine(w_value, 1), w_decay_down, w_rate_down], axis=1
    )
    w_conv = jnp.concatenate([mine(w_conv_gate, 1), mine(w_conv_in, 1), mine(w_conv_value, 1)], axis=1)
    w_out = jnp.concatenate([mine(w_out_conv, 0), mine(w_out_state, 0)], axis=0)
    shift = lax.all_to_all(
        decay_shift[0].reshape(steps, n_fs, width), "fs", split_axis=1, concat_axis=0
    ).reshape(n_fs, steps, width)
    shift, local_tokens = lax.optimization_barrier((shift, normalize_rows(norm_gain, tokens[0])))
    gathered = gather_inputs(n_sp, n_fs, n_tp, local_tokens, w_state)
    normed, w_state, w_conv, w_out = lax.optimization_barrier((*gathered, w_conv, w_out))
    normed = normed.reshape(n_fs * steps, normed.shape[-1])
    w_state = w_state.reshape(-1, w_state.shape[-1])
    w_conv = lax.all_gather(w_conv, "sp", axis=0, tiled=True)
    w_out = lax.all_gather(w_out, "sp", axis=0)

    state_in = jnp.dot(normed, w_state, preferred_element_type=f32).astype(bf16)
    params = jnp.stack([mine(p, 0) for p in (decay_base, rate_base, key_scale, key_mix)])
    rank = w_decay_down.shape[1]
    col = lambda k: pl.BlockSpec((steps, width), lambda i, k=k: (i, k))
    low = lambda k: pl.BlockSpec((steps, rank), lambda i, k=k: (i, 3 * width // rank + k))
    full = lambda s: pl.BlockSpec(s, lambda i: (0,) * len(s))
    query, local, ma = pl.pallas_call(
        state_kernel,
        grid=(n_fs,),
        in_specs=[
            col(0), col(1), col(2), low(0), low(1), full((rank, width)), full((rank, width)),
            pl.BlockSpec((1, steps, width), lambda i: (i, 0, 0)), full((4, width)),
        ],
        out_specs=[
            col(0), col(0), pl.BlockSpec((1, 2, HEAD, width), lambda i: (i, 0, 0, 0)),
        ],
        out_shape=[
            jax.ShapeDtypeStruct((n_fs * steps, width), bf16),
            jax.ShapeDtypeStruct((n_fs * steps, width), f32),
            jax.ShapeDtypeStruct((n_fs, 2, HEAD, width), bf16),
        ],
        cost_estimate=pl.CostEstimate(flops=40_000_000_000, bytes_accessed=4_000_000, transcendentals=0),
    )(
        state_in, state_in, state_in, state_in, state_in, mine(w_decay_up, 1), mine(w_rate_up, 1),
        shift, params,
    )
    ma_all = lax.all_gather(ma, "sp", axis=0)

    conv = jnp.dot(normed, w_conv, preferred_element_type=f32).astype(bf16)
    gate, source, value = (
        conv[:, i * width : (i + 1) * width].reshape(n_fs, steps, width) for i in range(3)
    )
    route = [(i, i + 1) for i in range(n_sp - 1)]
    previous = lax.ppermute(jnp.stack([source[:, -2:], value[:, -2:]]), "sp", route)
    product = jnp.concatenate([previous[0], source], axis=1).astype(f32) * jnp.concatenate(
        [previous[1], value], axis=1
    ).astype(f32)
    taps = mine(conv_taps, 1)
    filtered = taps[0] * product[:, :-2] + taps[1] * product[:, 1:-1] + taps[2] * product[:, 2:]
    conv_out = (gate.astype(f32) * filtered).astype(bf16).reshape(n_fs * steps, width)

    state_out = pl.pallas_call(
        functools.partial(finish_kernel, n_sp),
        grid=(n_fs,),
        in_specs=[
            pl.BlockSpec(memory_space=pltpu.SMEM), col(0), col(0),
            pl.BlockSpec((n_sp, 1, 2, HEAD, width), lambda i: (0, i, 0, 0, 0)), full((1, width)),
        ],
        out_specs=col(0),
        out_shape=jax.ShapeDtypeStruct((n_fs * steps, width), bf16),
    )(lax.axis_index("sp").reshape(1), query, local, ma_all, mine(group_gain, 0)[None])

    both = jnp.concatenate([conv_out, state_out], axis=1)
    w_out = jnp.swapaxes(w_out, 0, 1).reshape(both.shape[1], -1)
    partial = jnp.dot(both, w_out, preferred_element_type=f32).astype(bf16)
    mixed = reduce_partials(n_fs, partial.reshape(n_fs, n_tp, steps // n_tp, partial.shape[1]))
    return mixed[None]


def solution(mesh):
    in_specs = (
        P("fs", ("sp", "tp"), None), P(), P("sp", "tp"), P("sp", "tp"), P("sp", "tp"),
        P(None, "tp"), P("sp", "tp"), P("sp", "tp"), P("sp", "tp"), P("sp", None), P(None, "tp"),
        P("tp"), P("fs", "sp", "tp"), P("sp", None), P(None, "tp"), P("tp"), P("tp"), P("tp"),
        P("tp"), P("tp", "sp"), P("tp", "sp"),
    )
    out_specs = P("fs", ("sp", "tp"), None)
    return jax.shard_map(body, mesh=mesh, in_specs=in_specs, out_specs=out_specs, check_vma=False)
```

```python
import functools

import jax
import jax.numpy as jnp
from jax import lax
from jax.experimental import pallas as pl
from jax.experimental.pallas import tpu as pltpu
from jax.sharding import PartitionSpec as P

HEAD = 64
CHUNK = 64
norm_eps = 1e-06
group_eps = 0.00064
f32, bf16 = jnp.float32, jnp.bfloat16

NN = (((1,), (0,)), ((), ()))
NT = (((1,), (1,)), ((), ()))
TN = (((0,), (0,)), ((), ()))


def dot1(a, b, dims):
    return lax.dot_general(a.astype(bf16), b.astype(bf16), dims, preferred_element_type=f32)


def dot3(a, b, dims):
    ah, bh = a.astype(bf16), b.astype(bf16)
    al, bl = (a - ah.astype(f32)).astype(bf16), (b - bh.astype(f32)).astype(bf16)
    d = functools.partial(lax.dot_general, dimension_numbers=dims, preferred_element_type=f32)
    return d(ah, bh) + (d(ah, bl) + d(al, bh))


def stack_heads(x, lanes_low):
    return jnp.concatenate([jnp.where(lanes_low, x, 0.0), jnp.where(lanes_low, 0.0, x)], axis=0)


def fold(x):
    half = x.shape[0] // 2
    return x[:half] + x[half:]


def state_kernel(
    recv_ref, key_ref, val_ref, dlow_ref, rlow_ref, wdu_ref, wru_ref, shift_ref, par_ref,
    q_ref, l_ref, ma_ref,
):
    tokens, width = recv_ref.shape
    par = par_ref[...]
    decay_base, rate_base, key_scale, key_mix = (par[i : i + 1] for i in range(4))
    act = jnp.tanh(dlow_ref[...].astype(f32)).astype(bf16)
    pre = decay_base + lax.dot_general(act, wdu_ref[...], NN, preferred_element_type=f32)
    log_decay = shift_ref[0] - jnp.exp(-0.5) * jax.nn.sigmoid(pre)
    rate = jax.nn.sigmoid(
        rate_base + lax.dot_general(rlow_ref[...], wru_ref[...], NN, preferred_element_type=f32)
    )
    key = key_ref[...].astype(f32)
    scaled = key * key_scale
    lane_low = lax.broadcasted_iota(jnp.int32, (1, width), 1) < HEAD
    sq = scaled * scaled
    low_sum = jnp.sum(jnp.where(lane_low, sq, 0.0), axis=-1, keepdims=True)
    high_sum = jnp.sum(jnp.where(lane_low, 0.0, sq), axis=-1, keepdims=True)
    erase = scaled * lax.rsqrt(jnp.where(lane_low, low_sum, high_sum) + norm_eps)
    write = key * (1.0 + (rate - 1.0) * key_mix)
    replace = erase * rate
    recv = recv_ref[...].astype(f32)
    val = val_ref[...].astype(f32)

    rows = 2 * CHUNK
    ri = lax.broadcasted_iota(jnp.int32, (rows, rows), 0)
    ci = lax.broadcasted_iota(jnp.int32, (rows, rows), 1)
    same = (ri < CHUNK) == (ci < CHUNK)
    strict = jnp.logical_and(same, ri > ci)
    causal = jnp.logical_and(same, ri >= ci)
    eye = (ri == ci).astype(f32)
    tri = jnp.where(
        lax.broadcasted_iota(jnp.int32, (CHUNK, CHUNK), 0)
        >= lax.broadcasted_iota(jnp.int32, (CHUNK, CHUNK), 1),
        1.0,
        0.0,
    ).astype(f32)
    wi = lax.broadcasted_iota(jnp.int32, (width, width), 0)
    wj = lax.broadcasted_iota(jnp.int32, (width, width), 1)
    weye = wi == wj

    parts = []
    for c in range(tokens // CHUNK):
        sl = slice(c * CHUNK, (c + 1) * CHUNK)
        ld = log_decay[sl]
        incl = lax.dot_general(tri, ld, NN, precision=lax.Precision.HIGHEST, preferred_element_type=f32)
        final = incl[CHUNK - 1 : CHUNK]
        mid = incl[CHUNK // 2 - 1 : CHUNK // 2]
        excl = incl - ld
        up, back = jnp.exp(incl - mid), jnp.exp(mid - incl)
        st = lambda x: stack_heads(x, lane_low)
        e_mid = st(-erase[sl] * jnp.exp(excl - mid))
        q_mid = st(recv[sl] * up)
        r_back = st(replace[sl] * back)
        k_back = st(write[sl] * back)
        v = st(val[sl])
        e_now = st(-erase[sl] * jnp.exp(excl))
        q_now = st(recv[sl] * jnp.exp(incl))
        tail = jnp.exp(final - incl)
        r_end = st(replace[sl] * tail)
        k_end = st(write[sl] * tail)
        pairs = dot1(
            jnp.concatenate([e_mid, q_mid], axis=0), jnp.concatenate([r_back, k_back], axis=0), NT
        )
        x = jnp.where(strict, pairs[:rows, :rows], 0.0)
        ek = jnp.where(strict, pairs[:rows, rows:], 0.0)
        qr = jnp.where(causal, pairs[rows:, :rows], 0.0)
        qk = jnp.where(causal, pairs[rows:, rows:], 0.0)
        ekv_qkv = dot1(jnp.concatenate([ek, qk], axis=0), v, NN)
        inv = eye + x
        power = dot1(x, x, NN)
        reached = 2
        while reached < CHUNK:
            if reached * 2 < CHUNK:
                step = dot1(jnp.concatenate([inv, power], axis=0), power, NN)
                inv, power = inv + step[:rows], step[rows:]
            else:
                inv = inv + dot1(inv, power, NN)
            reached *= 2
        solved = dot1(inv, jnp.concatenate([e_now, ekv_qkv[:rows]], axis=1), NN)
        start_map, local_erase = solved[:, :width], solved[:, width:]
        seen = dot1(qr, solved, NN)
        query_map = fold(q_now + seen[:, :width])
        local_out = fold(seen[:, width:] + ekv_qkv[rows:])
        decay_diag = jnp.where(weye, jnp.exp(final), 0.0)
        step_map = decay_diag + dot3(start_map, r_end, TN)
        carried = dot1(local_erase, r_end, TN) + dot1(v, k_end, TN)
        parts.append((query_map, local_out, step_map, carried))

    total_map = total_add = None
    for c, (query_map, local_out, step_map, carried) in enumerate(parts):
        sl = slice(c * CHUNK, (c + 1) * CHUNK)
        if c == 0:
            q_ref[sl] = query_map.astype(bf16)
            l_ref[sl] = local_out
            total_map, total_add = step_map, carried
        else:
            q_ref[sl] = dot1(query_map, total_map, NT).astype(bf16)
            l_ref[sl] = local_out + dot1(query_map, total_add, NT)
            total_map, total_add = (
                dot3(total_map, step_map, NN),
                dot3(total_add, step_map, NN) + carried,
            )
    ma_ref[0, 0] = fold(total_map).astype(bf16)
    ma_ref[0, 1] = fold(total_add).astype(bf16)


def finish_kernel(n_sp, place_ref, q_ref, l_ref, ma_ref, gain_ref, out_ref):
    width = q_ref.shape[1]
    place = place_ref[0]
    wi = lax.broadcasted_iota(jnp.int32, (width, width), 0)
    wj = lax.broadcasted_iota(jnp.int32, (width, width), 1)
    same = (wi < HEAD) == (wj < HEAD)
    widen = lambda x: jnp.where(same, jnp.concatenate([x, x], axis=0), 0.0)
    state = jnp.zeros((width, width), f32)
    for hop in range(n_sp - 1):
        new = dot3(state, widen(ma_ref[hop, 0, 0].astype(f32)), NN) + widen(
            ma_ref[hop, 0, 1].astype(f32)
        )
        state = jnp.where(hop < place, new, state)
    out = l_ref[...] + dot1(q_ref[...], state, NT)
    low = lax.broadcasted_iota(jnp.int32, (1, width), 1) < HEAD

    def head_mean(x):
        a = jnp.sum(jnp.where(low, x, 0.0), axis=-1, keepdims=True)
        b = jnp.sum(jnp.where(low, 0.0, x), axis=-1, keepdims=True)
        return jnp.where(low, a, b) * (1.0 / HEAD)

    centered = out - head_mean(out)
    var = head_mean(centered * centered)
    out_ref[...] = (centered * lax.rsqrt(var + group_eps) * gain_ref[...]).astype(bf16)


MESH = pl.DeviceIdType.MESH


def greet(peers):
    barrier = pltpu.get_barrier_semaphore()
    for peer in peers:
        pl.semaphore_signal(barrier, inc=1, device_id=peer, device_id_type=MESH)
    return barrier


def send(src, dst, send_sem, recv_sem, peer):
    return pltpu.make_async_remote_copy(
        src_ref=src, dst_ref=dst, send_sem=send_sem, recv_sem=recv_sem,
        device_id=peer, device_id_type=MESH,
    )


def gather_kernel(
    n_sp, n_fs, tok_ref, shift_ref, *refs
):
    w_refs, refs = refs[:5], refs[5:]
    (
        toks, weights, shifts, w_sem, local_sem, tok_send, tok_recv, pair_send, pair_recv,
        right_send, left_send, w_recv, shift_send, shift_recv,
    ) = refs
    width = shifts.shape[-1]
    sp, fs, tp = lax.axis_index("sp"), lax.axis_index("fs"), lax.axis_index("tp")
    partner = {"tp": 1 - tp}
    others = [lax.rem(fs + d, n_fs) for d in range(1, n_fs)]
    start_lane, pieces = 0, []
    for k, ref in enumerate(w_refs):
        wide = width if k < 3 else ref.shape[1]
        source = ref.at[:, pl.ds(pl.multiple_of(fs * width, width), width)] if k < 3 else ref
        pieces.append(
            pltpu.make_async_copy(
                source, weights.at[sp, :, pl.ds(start_lane, wide)], w_sem.at[k]
            )
        )
        start_lane += wide
    for piece in pieces:
        piece.start()

    def shift_block(f):
        return shift_ref.at[:, pl.ds(pl.multiple_of(f * width, width), width)]

    barrier = greet([partner] + [{"fs": f} for f in others])
    has_left, has_right = sp > 0, sp < n_sp - 1

    @pl.when(has_left)
    def _():
        pl.semaphore_signal(barrier, inc=1, device_id={"sp": sp - 1}, device_id_type=MESH)

    @pl.when(has_right)
    def _():
        pl.semaphore_signal(barrier, inc=1, device_id={"sp": sp + 1}, device_id_type=MESH)

    pl.semaphore_wait(barrier, n_fs + has_left.astype(jnp.int32) + has_right.astype(jnp.int32))

    def rightward(j):
        src = weights.at[j]
        return send(src, weights.at[j], right_send.at[j], w_recv.at[j], {"sp": sp + 1})

    def leftward(j):
        src = weights.at[j]
        return send(src, weights.at[j], left_send.at[j], w_recv.at[j], {"sp": sp - 1})

    own_right, own_left = rightward(sp), leftward(sp)
    for piece in pieces:
        piece.wait()

    @pl.when(has_right)
    def _():
        own_right.start()

    @pl.when(has_left)
    def _():
        own_left.start()

    own_s = pltpu.make_async_copy(shift_block(fs), shifts.at[fs], local_sem.at[0])
    own_t = pltpu.make_async_copy(tok_ref, toks.at[fs, tp], local_sem.at[1])
    own_s.start()
    own_t.start()
    token_sends = [
        send(tok_ref, toks.at[fs, tp], tok_send.at[f], tok_recv.at[fs], {"fs": f}) for f in others
    ]
    for copy in token_sends:
        copy.start()
    pair_own = send(tok_ref, toks.at[fs, tp], pair_send.at[fs], pair_recv.at[fs], partner)
    pair_own.start()
    shift_sends = [
        send(shift_block(f), shifts.at[fs], shift_send.at[f], shift_recv.at[fs], {"fs": f})
        for f in others
    ]
    for copy in shift_sends:
        copy.start()

    def from_peer(f):
        return send(toks.at[f, tp], toks.at[f, tp], tok_send.at[f], tok_recv.at[f], {"fs": f})

    def to_partner(f):
        return send(toks.at[f, tp], toks.at[f, tp], pair_send.at[f], pair_recv.at[f], partner)

    def from_partner(f):
        there = toks.at[f, 1 - tp]
        return send(there, there, pair_send.at[f], pair_recv.at[f], partner)

    for k in range(1, n_sp):

        @pl.when(sp >= k)
        def _():
            rightward(sp - k).wait_recv()

            @pl.when(has_right)
            def _():
                rightward(sp - k).start()

        @pl.when(sp + k < n_sp)
        def _():
            leftward(sp + k).wait_recv()

            @pl.when(has_left)
            def _():
                leftward(sp + k).start()

        if k == 1:
            for f in reversed(others):
                from_peer(f).wait_recv()
                to_partner(f).start()

    own_s.wait()
    own_t.wait()
    for copy in token_sends + shift_sends:
        copy.wait_send()
    for f in others:
        send(shifts.at[f], shifts.at[f], shift_send.at[f], shift_recv.at[f], {"fs": f}).wait_recv()
    pair_own.wait_send()
    for f in others:
        to_partner(f).wait_send()
    for f in [fs] + others:
        from_partner(f).wait_recv()

    @pl.when(has_right)
    def _():
        own_right.wait_send()

    @pl.when(has_left)
    def _():
        own_left.wait_send()

    for k in range(1, n_sp):

        @pl.when(jnp.logical_and(sp >= k, has_right))
        def _():
            rightward(sp - k).wait_send()

        @pl.when(jnp.logical_and(sp + k < n_sp, has_left))
        def _():
            leftward(sp + k).wait_send()


def reduce_kernel(
    n_fs, part_ref, out_ref, from_pair, sums, from_fs, pair_send, pair_recv, fs_send, fs_recv
):
    fs, tp = lax.axis_index("fs"), lax.axis_index("tp")
    partner = {"tp": 1 - tp}
    order = [lax.rem(fs + d, n_fs) for d in range(1, n_fs)] + [fs]
    barrier = greet([partner] + [{"fs": f} for f in order[:-1]])
    pl.semaphore_wait(barrier, n_fs)
    swaps = [
        send(part_ref.at[f, 1 - tp], from_pair.at[d], pair_send.at[d], pair_recv.at[d], partner)
        for d, f in enumerate(order)
    ]
    for copy in swaps:
        copy.start()
    sends = []
    for d, f in enumerate(order):
        swaps[d].wait_recv()
        total = part_ref[f, tp].astype(f32) + from_pair[d].astype(f32)
        sums[d] = total.astype(bf16)
        if d < n_fs - 1:
            copy = send(sums.at[d], from_fs.at[d], fs_send.at[d], fs_recv.at[d], {"fs": f})
            copy.start()
            sends.append(copy)
    for copy in sends:
        copy.wait_recv()
    result = sums[n_fs - 1].astype(f32)
    for d in range(n_fs - 1):
        result = result + from_fs[d].astype(f32)
    out_ref[...] = result.astype(bf16)
    for copy in sends:
        copy.wait_send()
    for copy in swaps:
        copy.wait_send()


def gather_inputs(n_sp, n_fs, n_tp, tok, shift, weights):
    dma = lambda n: pltpu.SemaphoreType.DMA((n,))
    depth, width = weights[0].shape[0], weights[0].shape[1] // n_fs
    columns = 3 * width + weights[3].shape[1] + weights[4].shape[1]
    vmem = pl.BlockSpec(memory_space=pltpu.VMEM)
    return pl.pallas_call(
        functools.partial(gather_kernel, n_sp, n_fs),
        in_specs=[vmem, vmem] + [pl.BlockSpec(memory_space=pl.ANY)] * 5,
        out_specs=[vmem] * 3,
        out_shape=[
            jax.ShapeDtypeStruct((n_fs, n_tp) + tok.shape, bf16),
            jax.ShapeDtypeStruct((n_sp, depth, columns), bf16),
            jax.ShapeDtypeStruct((n_fs, shift.shape[0], width), f32),
        ],
        scratch_shapes=[dma(5), dma(2)] + [dma(n_fs)] * 4 + [dma(n_sp)] * 3 + [dma(n_fs)] * 2,
        compiler_params=pltpu.CompilerParams(collective_id=0, has_side_effects=True),
    )(tok, shift, *weights)


def map_kernel(n_sp, ma_ref, out_ref, send_sem, recv_sem):
    sp = lax.axis_index("sp")
    barrier = pltpu.get_barrier_semaphore()
    for k in range(1, n_sp):

        @pl.when(sp >= k)
        def _():
            pl.semaphore_signal(barrier, inc=1, device_id={"sp": sp - k}, device_id_type=MESH)

    @pl.when(sp < n_sp - 1)
    def _():
        pl.semaphore_wait(barrier, n_sp - 1 - sp)

    def later(k):
        return send(ma_ref, out_ref.at[sp], send_sem.at[k], recv_sem.at[sp], {"sp": sp + k})

    for k in range(1, n_sp):

        @pl.when(sp + k < n_sp)
        def _():
            later(k).start()

    for k in range(1, n_sp):

        @pl.when(sp >= k)
        def _():
            slot = out_ref.at[sp - k]
            send(slot, slot, send_sem.at[0], recv_sem.at[sp - k], {"sp": sp - k}).wait_recv()

        @pl.when(sp + k < n_sp)
        def _():
            later(k).wait_send()


def earlier_maps(n_sp, ma):
    return pl.pallas_call(
        functools.partial(map_kernel, n_sp),
        in_specs=[pl.BlockSpec(memory_space=pltpu.VMEM)],
        out_specs=pl.BlockSpec(memory_space=pltpu.VMEM),
        out_shape=jax.ShapeDtypeStruct((n_sp,) + ma.shape, bf16),
        scratch_shapes=[pltpu.SemaphoreType.DMA((n_sp,))] * 2,
        compiler_params=pltpu.CompilerParams(collective_id=2, has_side_effects=True),
    )(ma)


def reduce_partials(n_fs, part):
    dma = pltpu.SemaphoreType.DMA((n_fs,))
    block = pltpu.VMEM((n_fs,) + part.shape[2:], bf16)
    return pl.pallas_call(
        functools.partial(reduce_kernel, n_fs),
        in_specs=[pl.BlockSpec(memory_space=pltpu.VMEM)],
        out_specs=pl.BlockSpec(memory_space=pltpu.VMEM),
        out_shape=jax.ShapeDtypeStruct(part.shape[2:], bf16),
        scratch_shapes=[block, block, block, dma, dma, dma, dma],
        compiler_params=pltpu.CompilerParams(collective_id=1, has_side_effects=True),
    )(part)


def normalize_rows(norm_gain, row_piece):
    values = row_piece.astype(f32)
    scaled = values * lax.rsqrt(jnp.mean(values * values, axis=-1, keepdims=True) + norm_eps)
    return (scaled * norm_gain).astype(bf16)


def body(
    tokens, norm_gain, w_conv_gate, w_conv_in, w_conv_value, conv_taps, w_receptance, w_key,
    w_value, w_decay_down, w_decay_up, decay_base, decay_shift, w_rate_down, w_rate_up,
    rate_base, key_scale, key_mix, group_gain, w_out_conv, w_out_state,
):
    n_fs, n_sp = lax.axis_size("fs"), lax.axis_size("sp")
    fs = lax.axis_index("fs")
    width = w_key.shape[1] // n_fs

    def mine(a, axis):
        return lax.dynamic_slice_in_dim(a, fs * width, width, axis)

    n_tp = lax.axis_size("tp")
    steps = decay_shift.shape[1]
    w_conv = jnp.concatenate([mine(w_conv_gate, 1), mine(w_conv_in, 1), mine(w_conv_value, 1)], axis=1)
    w_out = jnp.concatenate([mine(w_out_conv, 0), mine(w_out_state, 0)], axis=0)
    normed, w_state, shift = gather_inputs(
        n_sp, n_fs, n_tp, normalize_rows(norm_gain, tokens[0]), decay_shift[0],
        (w_receptance, w_key, w_value, w_decay_down, w_rate_down),
    )
    normed, w_state, w_conv, w_out = lax.optimization_barrier((normed, w_state, w_conv, w_out))
    normed = normed.reshape(n_fs * steps, normed.shape[-1])
    w_state = w_state.reshape(-1, w_state.shape[-1])
    w_conv = lax.all_gather(w_conv, "sp", axis=0, tiled=True)
    w_out = lax.all_gather(w_out, "sp", axis=0)

    state_in = jnp.dot(normed, w_state, preferred_element_type=f32).astype(bf16)
    params = jnp.stack([mine(p, 0) for p in (decay_base, rate_base, key_scale, key_mix)])
    rank = w_decay_down.shape[1]
    col = lambda k: pl.BlockSpec((steps, width), lambda i, k=k: (i, k))
    low = lambda k: pl.BlockSpec((steps, rank), lambda i, k=k: (i, 3 * width // rank + k))
    full = lambda s: pl.BlockSpec(s, lambda i: (0,) * len(s))
    query, local, ma = pl.pallas_call(
        state_kernel,
        grid=(n_fs,),
        in_specs=[
            col(0), col(1), col(2), low(0), low(1), full((rank, width)), full((rank, width)),
            pl.BlockSpec((1, steps, width), lambda i: (i, 0, 0)), full((4, width)),
        ],
        out_specs=[
            col(0), col(0), pl.BlockSpec((1, 2, HEAD, width), lambda i: (i, 0, 0, 0)),
        ],
        out_shape=[
            jax.ShapeDtypeStruct((n_fs * steps, width), bf16),
            jax.ShapeDtypeStruct((n_fs * steps, width), f32),
            jax.ShapeDtypeStruct((n_fs, 2, HEAD, width), bf16),
        ],
        cost_estimate=pl.CostEstimate(flops=40_000_000_000, bytes_accessed=4_000_000, transcendentals=0),
    )(
        state_in, state_in, state_in, state_in, state_in, mine(w_decay_up, 1), mine(w_rate_up, 1),
        shift, params,
    )
    ma_all = earlier_maps(n_sp, ma)

    conv = jnp.dot(normed, w_conv, preferred_element_type=f32).astype(bf16)
    gate, source, value = (
        conv[:, i * width : (i + 1) * width].reshape(n_fs, steps, width) for i in range(3)
    )
    route = [(i, i + 1) for i in range(n_sp - 1)]
    previous = lax.ppermute(jnp.stack([source[:, -2:], value[:, -2:]]), "sp", route)
    product = jnp.concatenate([previous[0], source], axis=1).astype(f32) * jnp.concatenate(
        [previous[1], value], axis=1
    ).astype(f32)
    taps = mine(conv_taps, 1)
    filtered = taps[0] * product[:, :-2] + taps[1] * product[:, 1:-1] + taps[2] * product[:, 2:]
    conv_out = (gate.astype(f32) * filtered).astype(bf16).reshape(n_fs * steps, width)

    state_out = pl.pallas_call(
        functools.partial(finish_kernel, n_sp),
        grid=(n_fs,),
        in_specs=[
            pl.BlockSpec(memory_space=pltpu.SMEM), col(0), col(0),
            pl.BlockSpec((n_sp, 1, 2, HEAD, width), lambda i: (0, i, 0, 0, 0)), full((1, width)),
        ],
        out_specs=col(0),
        out_shape=jax.ShapeDtypeStruct((n_fs * steps, width), bf16),
    )(lax.axis_index("sp").reshape(1), query, local, ma_all, mine(group_gain, 0)[None])

    both = jnp.concatenate([conv_out, state_out], axis=1)
    w_out = jnp.swapaxes(w_out, 0, 1).reshape(both.shape[1], -1)
    partial = jnp.dot(both, w_out, preferred_element_type=f32).astype(bf16)
    mixed = reduce_partials(n_fs, partial.reshape(n_fs, n_tp, steps // n_tp, partial.shape[1]))
    return mixed[None]


def solution(mesh):
    in_specs = (
        P("fs", ("sp", "tp"), None), P(), P("sp", "tp"), P("sp", "tp"), P("sp", "tp"),
        P(None, "tp"), P("sp", "tp"), P("sp", "tp"), P("sp", "tp"), P("sp", None), P(None, "tp"),
        P("tp"), P("fs", "sp", "tp"), P("sp", None), P(None, "tp"), P("tp"), P("tp"), P("tp"),
        P("tp"), P("tp", "sp"), P("tp", "sp"),
    )
    out_specs = P("fs", ("sp", "tp"), None)
    return jax.shard_map(body, mesh=mesh, in_specs=in_specs, out_specs=out_specs, check_vma=False)
```
